32 devices in a mesh: ep: 8 (over z, x), tp: 4 (over y, core).
Axes of the slice: x: 2, y: 2, z: 4, core: 2. Of those that a mesh axis runs over, the one named last changes fastest.
Arguments:
- hidden_in: bfloat16 [256, 2048], P('ep', 'tp'), may hold values from -6 to 6
- state_in: float32 [256, 8, 128, 128], P('ep', 'tp'), may hold values from -0.6 to 0.6
- attn_gain: float32 [2048], replicated, may hold values from 0.1 to 1.9
- w_query: bfloat16 [2048, 1024], P(None, 'tp'), may hold values from -0.125 to 0.125
- w_key: bfloat16 [2048, 1024], P(None, 'tp'), may hold values from -0.125 to 0.125
- w_value: bfloat16 [2048, 1024], P(None, 'tp'), may hold values from -0.125 to 0.125
- w_gate: bfloat16 [2048, 1024], P(None, 'tp'), may hold values from -0.125 to 0.125
- w_beta: bfloat16 [2048, 8], replicated, may hold values from -0.125 to 0.125
- w_decay: bfloat16 [2048, 8], replicated, may hold values from -0.125 to 0.125
- decay_scale: float32 [8], replicated, may hold values from 0.05 to 3
- head_gain: float32 [128], replicated, may hold values from 0.1 to 1.9
- w_output: bfloat16 [1024, 2048], P(None, 'tp'), may hold values from -0.1875 to 0.1875
- ffn_gain: float32 [2048], replicated, may hold values from 0.1 to 1.9
- expert_ids: int32 [256, 2], P('ep'), may hold values from 0 to 7, all different within a row; in each aligned block of 32 rows (0 to 31, 32 to 63, ...) at most 16 rows name the same one
- route_weight: float32 [256, 2], P('ep'), may hold values from 0.2 to 1
- expert_gate: bfloat16 [8, 2048, 3072], P('ep', None, 'tp'), may hold values from -0.125 to 0.125
- expert_up: bfloat16 [8, 2048, 3072], P('ep', None, 'tp'), may hold values from -0.125 to 0.125
- expert_down: bfloat16 [8, 3072, 2048], P('ep', 'tp'), may hold values from -0.109375 to 0.109375
- dense_gate: bfloat16 [2048, 4096], P(None, 'ep'), may hold values from -0.125 to 0.125
- dense_up: bfloat16 [2048, 4096], P(None, 'ep'), may hold values from -0.125 to 0.125
- dense_down: bfloat16 [4096, 2048], P('ep'), may hold values from -0.09375 to 0.09375
- dense_mix: float32 [2048], P('tp'), may hold values from -6 to 6
Outputs:
- result: bfloat16 [256, 2048], P('ep', 'tp')
- new_state: float32 [256, 8, 128, 128], P('ep', 'tp')
The draws below stay inside these ranges and needn't reach their ends.
Inputs may be any that keep to these rules, and one draw needn't show every extreme that they name: `expert_ids`: each row names 2 different experts. Within the rows of one index of ep (aligned blocks of 32 sequences) no expert is named more than 16 times, a bound that some block reaches.
All inputs are finite; a program needn't handle non-finite values.
Results may differ from the reference program's by a relative error of at most 0.015.
Values may be sent and summed in bfloat16 or wider, within the bound.
No kernel may reach another device: no remote copies, remote signals or barrier semaphores. Data moves between devices by JAX's collectives and lax.ppermute only.
A program may use at most 64 MiB of HBM per device.

```python
import math
import jax
import jax.numpy as jnp
import numpy as np
from jax import lax

D = 2048
H = 8
DK = 128
DV = 128
FE = 3072
FFD = 4096
TOP = 2
SEQ_DEV = 32
EXPERTS = 8
CAP = 16
SEQS = 256
N_EP = 8
N_TP = 4


def steps_of(key, dims, shards, least, largest):
    def one(position, shards_of):
        heights = jax.random.uniform(jax.random.fold_in(jax.random.fold_in(key, 6), position), (shards_of,), jnp.float32, least / len(shards), largest / len(shards))
        return jnp.repeat(jnp.exp(heights), dims[position] // shards_of).reshape((-1,) + (1,) * (len(dims) - position - 1))

    level = one(*shards[0])
    for cut in shards[1:]:
        level = level * one(*cut)
    return level


def deal_out(key, own, number, rows, count, top, reach, skew):
    sequence = jax.random.permutation(key, count)
    packed, ordinary = portions_of(count, rows * top, reach, skew, True), portions_of(count, rows * top, reach, skew, False)
    places = jnp.arange(count)

    def named(lengths, offset_by):
        used = int((lengths > 0).sum())
        fixed = max(1, used // 4)
        shifted = fixed + (places - fixed + offset_by * (used - fixed)) % max(1, count - fixed)
        return jnp.zeros((count,), jnp.int32).at[sequence[jnp.where(places < fixed, places, shifted)]].set(jnp.asarray(lengths, jnp.int32))

    lengths = jnp.where(number % 4 == 0, named(packed, number // 4), named(ordinary, number - number // 4 - 1))
    mixed = jax.random.permutation(jax.random.fold_in(own, 3), count)
    donor, receiver = mixed[0:count // 2 * 2:2], mixed[1:count // 2 * 2:2]
    slack = jnp.minimum(lengths[donor] - 1, reach - lengths[receiver]) // 2
    slack = jnp.where((donor == sequence[0]) | (receiver == sequence[0]) | (lengths[receiver] == 0), 0, jnp.maximum(slack, 0))
    shifted = jax.random.randint(jax.random.fold_in(own, 4), (count // 2,), 0, 1 << 20) % (slack + 1)
    lengths = lengths.at[donor].add(-shifted).at[receiver].add(shifted)
    members = jnp.searchsorted(jnp.cumsum(lengths), jnp.arange(rows * top), side="right").astype(jnp.int32)
    listing = members.reshape(top, rows).T
    listing = listing[jax.random.permutation(jax.random.fold_in(own, 1), rows)]
    offset_by = jax.random.randint(jax.random.fold_in(own, 2), (rows, 1), 0, top)
    return jnp.take_along_axis(listing, (jnp.arange(top)[None, :] + offset_by) % top, axis=1)


def portions_of(number_of, total, reach, skew, full):
    portions = [(1 << 20) // math.isqrt(grade ** skew) + 1 for grade in range(1, number_of + 1)]
    largest = reach if full else min(reach, max(-(-total // number_of), total * portions[0] // sum(portions)))
    least = 1 if total - largest >= number_of - 1 else 0
    holding, rest = [largest] + [least] * (number_of - 1), total - largest - least * (number_of - 1)
    while rest > 0:
        candidates = [i for i in range(1, number_of) if holding[i] < largest] or [i for i in range(1, number_of) if holding[i] < reach]
        pool, left = sum([portions[i] for i in candidates]), rest
        for i in candidates:
            extra = min(reach - holding[i], max(1, left * portions[i] // pool), rest)
            holding[i] = holding[i] + extra
            rest = rest - extra
    return np.array(holding)


def bell_draw(key, extent, spread, reach, cuts=(), kind=jnp.bfloat16):
    entries = jax.random.normal(key, extent, jnp.float32) * spread
    if len(cuts) > 0:
        entries = steps_of(key, extent, cuts, -0.22, 0.18) * entries
    return jnp.clip(entries, min=-reach, max=reach).astype(kind)


def setup_inputs(seed: int = 0) -> dict:
    arg_keys = jax.random.split(jax.random.key(seed), 23)
    hidden_in = bell_draw(arg_keys[0], (SEQS, D), 1.0, 6.0, ((0, 8), (1, 4)))
    state_in = bell_draw(arg_keys[1], (SEQS, H, DK, DV), 0.09, 0.6, ((0, 8), (1, 4)), jnp.float32)
    attn_gain = jnp.clip(1.0 + 0.18 * jax.random.normal(arg_keys[2], (D,), jnp.float32), 0.1, 1.9)
    w_query = bell_draw(arg_keys[3], (D, H * DK), D ** -0.5, 0.125, ((1, 4),))
    w_key = bell_draw(arg_keys[4], (D, H * DK), D ** -0.5, 0.125, ((1, 4),))
    w_value = bell_draw(arg_keys[5], (D, H * DV), D ** -0.5, 0.125, ((1, 4),))
    w_gate = bell_draw(arg_keys[6], (D, H * DV), D ** -0.5, 0.125, ((1, 4),))
    w_beta = bell_draw(arg_keys[7], (D, H), D ** -0.5, 0.125)
    w_decay = bell_draw(arg_keys[8], (D, H), D ** -0.5, 0.125)
    decay_scale = jnp.clip(jnp.exp(jax.random.uniform(arg_keys[9], (H,), jnp.float32, math.log(0.05), math.log(3.0))), 0.05, 3.0)
    head_gain = jnp.clip(1.0 + 0.18 * jax.random.normal(arg_keys[10], (DV,), jnp.float32), 0.1, 1.9)
    w_output = bell_draw(arg_keys[11], (H * DV, D), (H * DV) ** -0.5, 0.1875, ((1, 4),))
    ffn_gain = jnp.clip(1.0 + 0.18 * jax.random.normal(arg_keys[12], (D,), jnp.float32), 0.1, 1.9)
    expert_ids_keys = jax.random.split(jax.random.fold_in(arg_keys[13], 1), SEQS // SEQ_DEV)
    expert_ids_turns = jax.random.permutation(jax.random.fold_in(arg_keys[13], 3), SEQS // SEQ_DEV)
    expert_ids = jax.vmap(lambda own, number: deal_out(jax.random.fold_in(arg_keys[13], 2), own, number, SEQ_DEV, EXPERTS, TOP, CAP, 2))(expert_ids_keys, expert_ids_turns).reshape((SEQS, TOP))
    route_weight = jnp.clip(jnp.exp(math.log(1.0) - 1.609438 * jax.random.uniform(arg_keys[14], (SEQS, TOP), jnp.float32) ** steps_of(arg_keys[14], (SEQS, TOP), ((0, 8),), -0.2, 0.2)), 0.2, 1.0)
    expert_gate = bell_draw(arg_keys[15], (EXPERTS, D, FE), D ** -0.5, 0.125, ((0, 8), (2, 4)))
    expert_up = bell_draw(arg_keys[16], (EXPERTS, D, FE), D ** -0.5, 0.125, ((0, 8), (2, 4)))
    expert_down = bell_draw(arg_keys[17], (EXPERTS, FE, D), FE ** -0.5, 0.109375, ((0, 8), (1, 4)))
    dense_gate = bell_draw(arg_keys[18], (D, FFD), D ** -0.5, 0.125, ((1, 8),))
    dense_up = bell_draw(arg_keys[19], (D, FFD), D ** -0.5, 0.125, ((1, 8),))
    dense_down = bell_draw(arg_keys[20], (FFD, D), FFD ** -0.5, 0.09375, ((0, 8),))
    dense_mix = bell_draw(arg_keys[21], (D,), 1.5, 6.0, ((0, 4),), jnp.float32)
    return dict(hidden_in=hidden_in, state_in=state_in, attn_gain=attn_gain, w_query=w_query, w_key=w_key, w_value=w_value, w_gate=w_gate, w_beta=w_beta, w_decay=w_decay, decay_scale=decay_scale, head_gain=head_gain, w_output=w_output, ffn_gain=ffn_gain, expert_ids=expert_ids, route_weight=route_weight, expert_gate=expert_gate, expert_up=expert_up, expert_down=expert_down, dense_gate=dense_gate, dense_up=dense_up, dense_down=dense_down, dense_mix=dense_mix)


EPS = 1e-06

def root_norm(values, scale_vec):
    wide = values.astype(jnp.float32)
    return wide * lax.rsqrt(lax.optimization_barrier(jnp.mean(wide * wide, axis=-1, keepdims=True)) + EPS) * scale_vec.astype(jnp.float32)

def unit_norm(values):
    return values * lax.rsqrt(lax.optimization_barrier(jnp.sum(values * values, axis=-1, keepdims=True)) + EPS)

def slot_table(expert_ids, count):
    flat = expert_ids.reshape(-1)
    onehot = (flat[:, None] == jnp.arange(count, dtype=jnp.int32)[None, :]).astype(jnp.int32)
    before = jnp.cumsum(onehot, axis=0) - onehot
    return lax.optimization_barrier(jnp.sum(before * onehot, axis=1)).reshape(expert_ids.shape)

def delta_update(old_state, key_rows, value_rows, beta_rate, decay_rate):
    recalled = jnp.einsum('shk,shkv->shv', key_rows, old_state, precision=lax.Precision.HIGHEST)
    erased = old_state - beta_rate[..., None, None] * key_rows[..., :, None] * recalled[..., None, :]
    written = beta_rate[..., None, None] * key_rows[..., :, None] * value_rows[..., None, :]
    return decay_rate[..., None, None] * erased + written

def head_output(new_state, queries, gate_rows, head_gain):
    read = jnp.einsum('shk,shkv->shv', queries, new_state, precision=lax.Precision.HIGHEST)
    return (root_norm(read, head_gain) * jax.nn.silu(gate_rows)).astype(jnp.bfloat16)

def reference(hidden_in, state_in, attn_gain, w_query, w_key, w_value, w_gate, w_beta, w_decay, decay_scale, head_gain, w_output, ffn_gain, expert_ids, route_weight, expert_gate, expert_up, expert_down, dense_gate, dense_up, dense_down, dense_mix):
    seqs = hidden_in.shape[0]
    normed = root_norm(hidden_in, attn_gain).astype(jnp.bfloat16)
    queries = unit_norm(jnp.dot(normed, w_query, preferred_element_type=jnp.float32).reshape(seqs, H, DK)) * DK ** (-0.5)
    key_rows = unit_norm(jnp.dot(normed, w_key, preferred_element_type=jnp.float32).reshape(seqs, H, DK))
    value_rows = jnp.dot(normed, w_value, preferred_element_type=jnp.float32).reshape(seqs, H, DV)
    gate_rows = jnp.dot(normed, w_gate, preferred_element_type=jnp.float32).reshape(seqs, H, DV)
    beta_rate = jax.nn.sigmoid(jnp.dot(normed, w_beta, preferred_element_type=jnp.float32))
    decay_logit = jnp.dot(normed, w_decay, preferred_element_type=jnp.float32)
    decay_rate = jnp.exp(-decay_scale[None, :] * jax.nn.softplus(decay_logit))
    new_state = delta_update(state_in, key_rows, value_rows, beta_rate, decay_rate)
    heads_out = head_output(new_state, queries, gate_rows, head_gain).reshape(seqs, H * DV)
    mixed = (hidden_in.astype(jnp.float32) + jnp.dot(heads_out, w_output, preferred_element_type=jnp.float32)).astype(jnp.bfloat16)
    normed2 = root_norm(mixed, ffn_gain).astype(jnp.bfloat16)
    groups = expert_ids.reshape(N_EP, SEQ_DEV, TOP)
    slots = jax.vmap(lambda group_ids: slot_table(group_ids, EXPERTS))(groups).reshape(seqs, TOP)
    group_index = (jnp.arange(seqs, dtype=jnp.int32) // SEQ_DEV)[:, None]
    place = (group_index * CAP + slots).astype(jnp.int32)
    spread_rows = jnp.broadcast_to(normed2[:, None, :], (seqs, TOP, D))
    buffer = jnp.zeros((EXPERTS, N_EP * CAP, D), jnp.bfloat16).at[expert_ids, place].set(spread_rows)

    def one_expert(operands):
        rows, gate_weight, up_weight, down_weight = operands
        gate_val = jnp.dot(rows, gate_weight, preferred_element_type=jnp.float32)
        up_val = jnp.dot(rows, up_weight, preferred_element_type=jnp.float32)
        inner = (jax.nn.silu(gate_val) * up_val).astype(jnp.bfloat16)
        width = inner.shape[1] // N_TP
        total = jnp.zeros((rows.shape[0], D), jnp.float32)
        for section in range(N_TP):
            term = jnp.dot(inner[:, section * width:(section + 1) * width], down_weight[section * width:(section + 1) * width, :], preferred_element_type=jnp.float32)
            total = total + lax.optimization_barrier(term.astype(jnp.bfloat16)).astype(jnp.float32)
        return total.astype(jnp.bfloat16)
    expert_out = lax.map(one_expert, (buffer, expert_gate, expert_up, expert_down))
    picked = expert_out[expert_ids, place].astype(jnp.float32)
    moe_sum = lax.optimization_barrier(jnp.sum(route_weight[..., None] * picked, axis=1))
    dense_gate_val = jnp.dot(normed2, dense_gate, preferred_element_type=jnp.float32)
    dense_up_val = jnp.dot(normed2, dense_up, preferred_element_type=jnp.float32)
    dense_hidden = (jax.nn.silu(dense_gate_val) * dense_up_val).astype(jnp.bfloat16)
    dense_out = jnp.dot(dense_hidden, dense_down, preferred_element_type=jnp.float32)
    result = (mixed.astype(jnp.float32) + moe_sum + jax.nn.sigmoid(dense_mix)[None, :] * dense_out).astype(jnp.bfloat16)
    return (result, new_state)
```

```python
import jax
import jax.numpy as jnp
from jax import lax
from jax.sharding import PartitionSpec as P

EPS = 1e-06


def root_norm(values, scale_vec):
    wide = values.astype(jnp.float32)
    return wide * lax.rsqrt(jnp.mean(wide * wide, axis=-1, keepdims=True) + EPS) * scale_vec


def unit_norm(values):
    return values * lax.rsqrt(jnp.sum(values * values, axis=-1, keepdims=True) + EPS)


def rejoin(pieces, index):
    bit = 1
    while bit < len(pieces):
        odd = (index // bit) % 2 == 1
        pieces = [jnp.where(odd, pieces[i ^ bit], pieces[i]) for i in range(len(pieces))]
        bit *= 2
    return pieces


def flip(values, ep_shift, tp_shift):
    ep_size = lax.axis_size("ep")
    tp_size = lax.axis_size("tp")
    pairs = [
        (e * tp_size + t, (e ^ ep_shift) * tp_size + (t ^ tp_shift))
        for e in range(ep_size)
        for t in range(tp_size)
    ]
    return lax.ppermute(values, ("ep", "tp"), pairs)


def delta_update(old_state, key_rows, value_rows, beta_rate, decay_rate):
    recalled = jnp.einsum("shk,shkv->shv", key_rows, old_state, precision=lax.Precision.HIGHEST)
    erased = (
        old_state - beta_rate[..., None, None] * key_rows[..., :, None] * recalled[..., None, :]
    )
    written = beta_rate[..., None, None] * key_rows[..., :, None] * value_rows[..., None, :]
    return decay_rate[..., None, None] * erased + written


def head_output(new_state, queries, gate_rows, head_gain):
    read = jnp.einsum("shk,shkv->shv", queries, new_state, precision=lax.Precision.HIGHEST)
    return (root_norm(read, head_gain) * jax.nn.silu(gate_rows)).astype(jnp.bfloat16)


def per_device(
    hidden_in,
    state_in,
    attn_gain,
    w_query,
    w_key,
    w_value,
    w_gate,
    w_beta,
    w_decay,
    decay_scale,
    head_gain,
    w_output,
    ffn_gain,
    expert_ids,
    route_weight,
    expert_gate,
    expert_up,
    expert_down,
    dense_gate,
    dense_up,
    dense_down,
    dense_mix,
):
    seq_dev = hidden_in.shape[0]
    tp_size = lax.axis_size("tp")
    ep_size = lax.axis_size("ep")
    tp_index = lax.axis_index("tp")
    local_heads = state_in.shape[1]
    key_dim = state_in.shape[2]
    value_dim = state_in.shape[3]
    local_width = hidden_in.shape[1]
    full_rows = lax.all_gather(hidden_in, "tp", axis=1, tiled=True)
    normed = root_norm(full_rows, attn_gain).astype(jnp.bfloat16)
    queries = unit_norm(
        jnp.dot(normed, w_query, preferred_element_type=jnp.float32).reshape(
            seq_dev, local_heads, key_dim
        )
    ) * key_dim ** (-0.5)
    key_rows = unit_norm(
        jnp.dot(normed, w_key, preferred_element_type=jnp.float32).reshape(
            seq_dev, local_heads, key_dim
        )
    )
    value_rows = jnp.dot(normed, w_value, preferred_element_type=jnp.float32).reshape(
        seq_dev, local_heads, value_dim
    )
    gate_rows = jnp.dot(normed, w_gate, preferred_element_type=jnp.float32).reshape(
        seq_dev, local_heads, value_dim
    )
    head_start = tp_index * local_heads
    beta_all = jnp.dot(normed, w_beta, preferred_element_type=jnp.float32)
    decay_all = jnp.dot(normed, w_decay, preferred_element_type=jnp.float32)
    beta_rate = jax.nn.sigmoid(lax.dynamic_slice_in_dim(beta_all, head_start, local_heads, 1))
    decay_logit = lax.dynamic_slice_in_dim(decay_all, head_start, local_heads, 1)
    decay_local = lax.dynamic_slice_in_dim(decay_scale, head_start, local_heads, 0)
    decay_rate = jnp.exp(-decay_local[None, :] * jax.nn.softplus(decay_logit))
    new_state = delta_update(state_in, key_rows, value_rows, beta_rate, decay_rate)
    heads_out = head_output(new_state, queries, gate_rows, head_gain).reshape(
        seq_dev, local_heads * value_dim
    )
    all_heads = lax.all_gather(heads_out, "tp", axis=1, tiled=True)
    mixed = (
        hidden_in.astype(jnp.float32)
        + jnp.dot(all_heads, w_output, preferred_element_type=jnp.float32)
    ).astype(jnp.bfloat16)
    ep_index = lax.axis_index("ep")
    cores = 2
    ny = tp_size // cores
    nx = ny if ep_size % ny == 0 else 1
    nz = ep_size // nx
    core_index = tp_index % cores
    y_index = tp_index // cores
    mix_parts = [dense_mix] + [flip(dense_mix, 0, r) for r in range(1, tp_size)]
    mix_full = jax.nn.sigmoid(jnp.concatenate(rejoin(mix_parts, tp_index)))

    def routed(target):
        return jnp.sum(
            jnp.where(expert_ids == target, route_weight, 0.0), axis=1, keepdims=True
        )

    shares = {}
    for r in range(ep_size):
        share = routed(ep_index ^ r)
        shares[r] = share if r == 0 else flip(share, r, 0)
    share_rows = jnp.concatenate(
        [shares[dz * nx + dx] for dx in range(nx) for dz in range(nz)], axis=0
    )

    column = jnp.concatenate(
        [mixed] + [flip(mixed, dz * nx, 0) for dz in range(1, nz)], axis=0
    )
    blocks = []
    for dx in range(nx):
        line = []
        for dy in range(ny):
            near = column if dx + dy == 0 else flip(column, dx, dy * cores)
            line.append(rejoin([near, flip(near, 0, 1)], core_index))
        line = [[line[dy][c] for dy in range(ny)] for c in range(cores)]
        line = [rejoin(part, y_index) for part in line]
        blocks.append(
            jnp.concatenate([line[c][y] for y in range(ny) for c in range(cores)], axis=1)
        )
    mixed_full = jnp.concatenate(blocks, axis=0)
    normed2 = root_norm(mixed_full, ffn_gain).astype(jnp.bfloat16)

    part = dense_gate.shape[1] // tp_size
    my_gate = lax.dynamic_slice_in_dim(dense_gate, tp_index * part, part, 1)
    my_up = lax.dynamic_slice_in_dim(dense_up, tp_index * part, part, 1)
    my_down = lax.dynamic_slice_in_dim(dense_down, tp_index * part, part, 0)

    def hidden(gate_weight, up_weight):
        gate_val = jnp.dot(normed2, gate_weight, preferred_element_type=jnp.float32)
        up_val = jnp.dot(normed2, up_weight, preferred_element_type=jnp.float32)
        return jax.nn.silu(gate_val) * up_val

    inner = hidden(expert_gate[0], expert_up[0]).astype(jnp.bfloat16)
    dense_hidden = hidden(my_gate, my_up).astype(jnp.bfloat16)
    total = (
        share_rows * jnp.dot(inner, expert_down[0], preferred_element_type=jnp.float32)
        + mix_full[None, :] * jnp.dot(dense_hidden, my_down, preferred_element_type=jnp.float32)
    ).astype(jnp.bfloat16)

    total = total.reshape(total.shape[0], ny, cores, local_width)
    halves = rejoin([total[:, :, c] for c in range(cores)], core_index)
    over = flip(halves[1], 0, 1)
    both = (halves[0].astype(jnp.float32) + over.astype(jnp.float32)).astype(jnp.bfloat16)
    near = rejoin([both[:, y] for y in range(ny)], y_index)
    span = nz * seq_dev
    summed = 0.0
    for dx in range(nx):
        for dy in range(ny):
            piece = near[dy][dx * span : (dx + 1) * span]
            piece = piece if dx + dy == 0 else flip(piece, dx, dy * cores)
            summed = summed + piece.astype(jnp.float32)
    summed = summed.astype(jnp.bfloat16)
    result = mixed.astype(jnp.float32)
    for dz in range(nz):
        piece = summed[dz * seq_dev : (dz + 1) * seq_dev]
        piece = piece if dz == 0 else flip(piece, dz * nx, 0)
        result = result + piece.astype(jnp.float32)
    return (result.astype(jnp.bfloat16), new_state)


def solution(mesh):
    placed = (
        P("ep", "tp"),
        P("ep", "tp", None, None),
        P(),
        P(None, "tp"),
        P(None, "tp"),
        P(None, "tp"),
        P(None, "tp"),
        P(),
        P(),
        P(),
        P(),
        P(None, "tp"),
        P(),
        P("ep", None),
        P("ep", None),
        P("ep", None, "tp"),
        P("ep", None, "tp"),
        P("ep", "tp", None),
        P(None, "ep"),
        P(None, "ep"),
        P("ep", None),
        P("tp"),
    )
    return jax.shard_map(
        per_device,
        mesh=mesh,
        in_specs=placed,
        out_specs=(P("ep", "tp"), P("ep", "tp", None, None)),
        check_vma=False,
    )
```

```python
import jax
import jax.numpy as jnp
from jax import lax
from jax.experimental import pallas as pl
from jax.experimental.pallas import tpu as pltpu
from jax.sharding import PartitionSpec as P

EPS = 1e-06


def root_norm(values, scale_vec):
    wide = values.astype(jnp.float32)
    return wide * lax.rsqrt(jnp.mean(wide * wide, axis=-1, keepdims=True) + EPS) * scale_vec


def unit_norm(values):
    return values * lax.rsqrt(jnp.sum(values * values, axis=-1, keepdims=True) + EPS)


def rejoin(pieces, index):
    bit = 1
    while bit < len(pieces):
        odd = (index // bit) % 2 == 1
        pieces = [jnp.where(odd, pieces[i ^ bit], pieces[i]) for i in range(len(pieces))]
        bit *= 2
    return pieces


def rejoin_all(groups, index):
    turned = [rejoin(list(lane), index) for lane in zip(*groups)]
    return [list(group) for group in zip(*turned)]


def flip(values, ep_shift, tp_shift):
    ep_size = lax.axis_size("ep")
    tp_size = lax.axis_size("tp")
    pairs = [
        (e * tp_size + t, (e ^ ep_shift) * tp_size + (t ^ tp_shift))
        for e in range(ep_size)
        for t in range(tp_size)
    ]
    return lax.ppermute(values, ("ep", "tp"), pairs)


def whole(shape, dtype):
    return jax.ShapeDtypeStruct(shape, dtype)


def attend(
    index_ref,
    rows_ref,
    gain_ref,
    wq_ref,
    wk_ref,
    wv_ref,
    wg_ref,
    wb_ref,
    wd_ref,
    scale_ref,
    head_gain_ref,
    state_ref,
    heads_ref,
    new_ref,
):
    seqs, heads, key_dim, value_dim = state_ref.shape
    chunks = [rows_ref[i, :seqs].astype(jnp.float32) for i in range(rows_ref.shape[0])]
    wide = jnp.concatenate(chunks, axis=1)
    normed = root_norm(wide, gain_ref[...]).astype(jnp.bfloat16)

    def project(weight_ref):
        return jnp.dot(normed, weight_ref[...], preferred_element_type=jnp.float32)

    def project_rows(weight_ref):
        return lax.dot_general(
            normed,
            weight_ref[...],
            (((1,), (1,)), ((), ())),
            preferred_element_type=jnp.float32,
        )

    queries = project(wq_ref)
    keys = project(wk_ref)
    values = project(wv_ref)
    gates = project(wg_ref)
    beta_all = jax.nn.sigmoid(project_rows(wb_ref))
    logit = project_rows(wd_ref)
    soft = jnp.maximum(logit, 0.0) + jnp.log(1.0 + jnp.exp(-jnp.abs(logit)))
    decay_all = jnp.exp(-scale_ref[...] * soft)
    lane = lax.broadcasted_iota(jnp.int32, beta_all.shape, 1)
    for h in range(heads):
        mine = lane == index_ref[0] * heads + h
        beta = jnp.sum(jnp.where(mine, beta_all, 0.0), axis=1, keepdims=True)
        decay = jnp.sum(jnp.where(mine, decay_all, 0.0), axis=1, keepdims=True)
        spot = slice(h * key_dim, (h + 1) * key_dim)
        place = slice(h * value_dim, (h + 1) * value_dim)
        query = unit_norm(queries[:, spot]) * key_dim ** (-0.5)
        key = unit_norm(keys[:, spot])
        overlap = jnp.sum(query * key, axis=1, keepdims=True) * beta
        query_t = query.T
        key_t = key.T
        value = values[:, place]
        decay = jnp.broadcast_to(decay, value.shape)
        beta = jnp.broadcast_to(beta, value.shape)
        reads = []
        deltas = []
        for s in range(seqs):
            old = state_ref[s, h]
            key_col = key_t[:, s : s + 1]
            recalled = jnp.sum(old * key_col, axis=0, keepdims=True)
            asked = jnp.sum(old * query_t[:, s : s + 1], axis=0, keepdims=True)
            fade = decay[s : s + 1]
            delta = value[s : s + 1] - fade * recalled
            new_ref[s, h] = fade * old + key_col * (beta[s : s + 1] * delta)
            reads.append(asked)
            deltas.append(delta)
        read = decay * jnp.concatenate(reads, axis=0) + overlap * jnp.concatenate(deltas, axis=0)
        heads_ref[:, place] = (
            root_norm(read, head_gain_ref[...]) * jax.nn.silu(gates[:, place])
        ).astype(jnp.bfloat16)


def split_two(values):
    high = lax.reduce_precision(values, 8, 7)
    low = lax.reduce_precision(values - high, 8, 7)
    return high.astype(jnp.bfloat16), low.astype(jnp.bfloat16)


def per_device(
    hidden_in,
    state_in,
    attn_gain,
    w_query,
    w_key,
    w_value,
    w_gate,
    w_beta,
    w_decay,
    decay_scale,
    head_gain,
    w_output,
    ffn_gain,
    expert_ids,
    route_weight,
    expert_gate,
    expert_up,
    expert_down,
    dense_gate,
    dense_up,
    dense_down,
    dense_mix,
):
    seq_dev = hidden_in.shape[0]
    tp_size = lax.axis_size("tp")
    ep_size = lax.axis_size("ep")
    tp_index = lax.axis_index("tp")
    local_heads = state_in.shape[1]
    key_dim = state_in.shape[2]
    value_dim = state_in.shape[3]
    local_width = hidden_in.shape[1]
    mix_high, mix_low = split_two(dense_mix)
    pad_rows = jnp.zeros((14, local_width), jnp.bfloat16)
    packed = jnp.concatenate([hidden_in, mix_high[None], mix_low[None], pad_rows], axis=0)
    full_rows = lax.all_gather(packed, "tp", axis=0)
    mix_pair = full_rows[:, seq_dev : seq_dev + 2].astype(jnp.float32)
    mix_full = jax.nn.sigmoid(mix_pair[:, 0] + mix_pair[:, 1]).reshape(1, -1)
    vmem = pl.BlockSpec(memory_space=pltpu.VMEM)
    smem = pl.BlockSpec(memory_space=pltpu.SMEM)
    heads_out, new_state = pl.pallas_call(
        attend,
        out_shape=(
            whole((seq_dev, local_heads * value_dim), jnp.bfloat16),
            whole(state_in.shape, jnp.float32),
        ),
        in_specs=[smem] + [vmem] * 11,
        out_specs=(vmem, vmem),
        compiler_params=pltpu.CompilerParams(vmem_limit_bytes=28 * 2**20),
        name="attend",
    )(
        tp_index.reshape(1),
        full_rows,
        attn_gain[None],
        w_query,
        w_key,
        w_value,
        w_gate,
        w_beta.T,
        w_decay.T,
        decay_scale[None],
        head_gain[None],
        state_in,
    )
    all_heads = lax.all_gather(heads_out, "tp", axis=1, tiled=True)
    mixed = (
        hidden_in.astype(jnp.float32)
        + jnp.dot(all_heads, w_output, preferred_element_type=jnp.float32)
    ).astype(jnp.bfloat16)
    ep_index = lax.axis_index("ep")
    cores = 2
    ny = tp_size // cores
    nx = ny if ep_size % ny == 0 else 1
    nz = ep_size // nx
    core_index = tp_index % cores
    y_index = tp_index // cores
    weight_high, weight_low = split_two(route_weight)
    top_count = expert_ids.shape[1]
    side = jnp.concatenate(
        [
            expert_ids.astype(jnp.bfloat16),
            weight_high,
            weight_low,
            jnp.zeros((seq_dev, 128 - 3 * top_count), jnp.bfloat16),
        ],
        axis=1,
    )
    loaded = jnp.concatenate([mixed, side], axis=1)
    column = jnp.concatenate(
        [loaded] + [flip(loaded, dz * nx, 0) for dz in range(1, nz)], axis=0
    )
    sides = [column[:, local_width:]]
    bare = column[:, :local_width]
    blocks = []
    for dx in range(nx):
        line = []
        for dy in range(ny):
            near = bare if dx + dy == 0 else flip(column if dy == 0 else bare, dx, dy * cores)
            if dx > 0 and dy == 0:
                sides.append(near[:, local_width:])
                near = near[:, :local_width]
            line.append(rejoin([near, flip(near, 0, 1)], core_index))
        line = [[line[dy][c] for dy in range(ny)] for c in range(cores)]
        line = [rejoin(part, y_index) for part in line]
        blocks.append(
            jnp.concatenate([line[c][y] for y in range(ny) for c in range(cores)], axis=1)
        )
    mixed_full = jnp.concatenate(blocks, axis=0)
    side_rows = jnp.concatenate(sides, axis=0).astype(jnp.float32)
    share_rows = 0.0
    for k in range(top_count):
        weight = (
            side_rows[:, top_count + k : top_count + k + 1]
            + side_rows[:, 2 * top_count + k : 2 * top_count + k + 1]
        )
        named = side_rows[:, k : k + 1] == ep_index.astype(jnp.float32)
        share_rows = share_rows + jnp.where(named, weight, 0.0)
    normed2 = root_norm(mixed_full, ffn_gain).astype(jnp.bfloat16)

    part = dense_gate.shape[1] // tp_size
    my_gate = lax.dynamic_slice_in_dim(dense_gate, tp_index * part, part, 1)
    my_up = lax.dynamic_slice_in_dim(dense_up, tp_index * part, part, 1)
    my_down = lax.dynamic_slice_in_dim(dense_down, tp_index * part, part, 0)

    def hidden(gate_weight, up_weight):
        gate_val = jnp.dot(normed2, gate_weight, preferred_element_type=jnp.float32)
        up_val = jnp.dot(normed2, up_weight, preferred_element_type=jnp.float32)
        return jax.nn.silu(gate_val) * up_val

    inner = hidden(expert_gate[0], expert_up[0]).astype(jnp.bfloat16)
    dense_hidden = hidden(my_gate, my_up).astype(jnp.bfloat16)
    total = (
        share_rows * jnp.dot(inner, expert_down[0], preferred_element_type=jnp.float32)
        + mix_full * jnp.dot(dense_hidden, my_down, preferred_element_type=jnp.float32)
    ).astype(jnp.bfloat16)

    lots = [
        [
            total[:, (y * cores + c) * local_width : (y * cores + c + 1) * local_width]
            for c in range(cores)
        ]
        for y in range(ny)
    ]
    near = []
    for pair in rejoin_all(lots, y_index):
        pair = rejoin(pair, core_index)
        over = flip(pair[1], 0, 1)
        near.append((pair[0].astype(jnp.float32) + over.astype(jnp.float32)).astype(jnp.bfloat16))
    span = nz * seq_dev
    summed = 0.0
    for dx in range(nx):
        for dy in range(ny):
            piece = near[dy][dx * span : (dx + 1) * span]
            piece = piece if dx + dy == 0 else flip(piece, dx, dy * cores)
            summed = summed + piece.astype(jnp.float32)
    summed = summed.astype(jnp.bfloat16)
    result = mixed.astype(jnp.float32)
    for dz in range(nz):
        piece = summed[dz * seq_dev : (dz + 1) * seq_dev]
        piece = piece if dz == 0 else flip(piece, dz * nx, 0)
        result = result + piece.astype(jnp.float32)
    return (result.astype(jnp.bfloat16), new_state)


def solution(mesh):
    placed = (
        P("ep", "tp"),
        P("ep", "tp", None, None),
        P(),
        P(None, "tp"),
        P(None, "tp"),
        P(None, "tp"),
        P(None, "tp"),
        P(),
        P(),
        P(),
        P(),
        P(None, "tp"),
        P(),
        P("ep", None),
        P("ep", None),
        P("ep", None, "tp"),
        P("ep", None, "tp"),
        P("ep", "tp", None),
        P(None, "ep"),
        P(None, "ep"),
        P("ep", None),
        P("tp"),
    )
    return jax.shard_map(
        per_device,
        mesh=mesh,
        in_specs=placed,
        out_specs=(P("ep", "tp"), P("ep", "tp", None, None)),
        check_vma=False,
    )
```

```python
import jax
import jax.numpy as jnp
from jax import lax
from jax.experimental import pallas as pl
from jax.experimental.pallas import tpu as pltpu
from jax.sharding import PartitionSpec as P

EPS = 1e-06


def root_norm(values, scale_vec):
    wide = values.astype(jnp.float32)
    return wide * lax.rsqrt(jnp.mean(wide * wide, axis=-1, keepdims=True) + EPS) * scale_vec


def unit_norm(values):
    return values * lax.rsqrt(jnp.sum(values * values, axis=-1, keepdims=True) + EPS)


def rejoin(pieces, index):
    bit = 1
    while bit < len(pieces):
        odd = (index // bit) % 2 == 1
        pieces = [jnp.where(odd, pieces[i ^ bit], pieces[i]) for i in range(len(pieces))]
        bit *= 2
    return pieces


def rejoin_all(groups, index):
    turned = [rejoin(list(lane), index) for lane in zip(*groups)]
    return [list(group) for group in zip(*turned)]


def flip(values, ep_shift, tp_shift):
    ep_size = lax.axis_size("ep")
    tp_size = lax.axis_size("tp")
    pairs = [
        (e * tp_size + t, (e ^ ep_shift) * tp_size + (t ^ tp_shift))
        for e in range(ep_size)
        for t in range(tp_size)
    ]
    return lax.ppermute(values, ("ep", "tp"), pairs)


def whole(shape, dtype):
    return jax.ShapeDtypeStruct(shape, dtype)


def attend(
    index_ref,
    rows_ref,
    gain_ref,
    wb_ref,
    wd_ref,
    scale_ref,
    head_gain_ref,
    wq_hbm,
    wk_hbm,
    wv_hbm,
    wg_hbm,
    state_hbm,
    heads_ref,
    new_hbm,
    wq_ref,
    wk_ref,
    wv_ref,
    wg_ref,
    state_ref,
    new_ref,
    weight_sems,
    load_sems,
    store_sems,
):
    seqs, heads, key_dim, value_dim = state_ref.shape
    weights = ((wq_hbm, wq_ref), (wk_hbm, wk_ref), (wv_hbm, wv_ref), (wg_hbm, wg_ref))
    fetches = [
        pltpu.make_async_copy(far, near, weight_sems.at[i])
        for i, (far, near) in enumerate(weights)
    ]
    loads = [
        pltpu.make_async_copy(state_hbm.at[:, h], state_ref.at[:, h], load_sems.at[h])
        for h in range(heads)
    ]
    stores = [
        pltpu.make_async_copy(new_ref.at[:, h], new_hbm.at[:, h], store_sems.at[h])
        for h in range(heads)
    ]
    for copy in fetches + loads:
        copy.start()
    chunks = [rows_ref[i, :seqs].astype(jnp.float32) for i in range(rows_ref.shape[0])]
    wide = jnp.concatenate(chunks, axis=1)
    normed = root_norm(wide, gain_ref[...]).astype(jnp.bfloat16)

    def project(weight_ref):
        return jnp.dot(normed, weight_ref[...], preferred_element_type=jnp.float32)

    def project_rows(weight_ref):
        return lax.dot_general(
            normed,
            weight_ref[...],
            (((1,), (1,)), ((), ())),
            preferred_element_type=jnp.float32,
        )

    fetches[0].wait()
    queries = project(wq_ref)
    fetches[1].wait()
    keys = project(wk_ref)
    fetches[2].wait()
    values = project(wv_ref)
    fetches[3].wait()
    gates = project(wg_ref)
    beta_all = jax.nn.sigmoid(project_rows(wb_ref))
    logit = project_rows(wd_ref)
    soft = jnp.maximum(logit, 0.0) + jnp.log(1.0 + jnp.exp(-jnp.abs(logit)))
    decay_all = jnp.exp(-scale_ref[...] * soft)
    lane = lax.broadcasted_iota(jnp.int32, beta_all.shape, 1)
    for h in range(heads):
        mine = lane == index_ref[0] * heads + h
        beta = jnp.sum(jnp.where(mine, beta_all, 0.0), axis=1, keepdims=True)
        decay = jnp.sum(jnp.where(mine, decay_all, 0.0), axis=1, keepdims=True)
        spot = slice(h * key_dim, (h + 1) * key_dim)
        place = slice(h * value_dim, (h + 1) * value_dim)
        query = unit_norm(queries[:, spot]) * key_dim ** (-0.5)
        key = unit_norm(keys[:, spot])
        overlap = jnp.sum(query * key, axis=1, keepdims=True) * beta
        query_t = query.T
        key_t = key.T
        value = values[:, place]
        decay = jnp.broadcast_to(decay, value.shape)
        beta = jnp.broadcast_to(beta, value.shape)
        reads = []
        deltas = []
        loads[h].wait()
        for s in range(seqs):
            old = state_ref[s, h]
            key_col = key_t[:, s : s + 1]
            recalled = jnp.sum(old * key_col, axis=0, keepdims=True)
            asked = jnp.sum(old * query_t[:, s : s + 1], axis=0, keepdims=True)
            fade = decay[s : s + 1]
            delta = value[s : s + 1] - fade * recalled
            new_ref[s, h] = fade * old + key_col * (beta[s : s + 1] * delta)
            reads.append(asked)
            deltas.append(delta)
        stores[h].start()
        read = decay * jnp.concatenate(reads, axis=0) + overlap * jnp.concatenate(deltas, axis=0)
        heads_ref[:, place] = (
            root_norm(read, head_gain_ref[...]) * jax.nn.silu(gates[:, place])
        ).astype(jnp.bfloat16)
    for copy in stores:
        copy.wait()


def split_two(values):
    high = lax.reduce_precision(values, 8, 7)
    low = lax.reduce_precision(values - high, 8, 7)
    return high.astype(jnp.bfloat16), low.astype(jnp.bfloat16)


def per_device(
    hidden_in,
    state_in,
    attn_gain,
    w_query,
    w_key,
    w_value,
    w_gate,
    w_beta,
    w_decay,
    decay_scale,
    head_gain,
    w_output,
    ffn_gain,
    expert_ids,
    route_weight,
    expert_gate,
    expert_up,
    expert_down,
    dense_gate,
    dense_up,
    dense_down,
    dense_mix,
):
    seq_dev = hidden_in.shape[0]
    tp_size = lax.axis_size("tp")
    ep_size = lax.axis_size("ep")
    tp_index = lax.axis_index("tp")
    local_heads = state_in.shape[1]
    key_dim = state_in.shape[2]
    value_dim = state_in.shape[3]
    local_width = hidden_in.shape[1]
    mix_high, mix_low = split_two(dense_mix)
    pad_rows = jnp.zeros((14, local_width), jnp.bfloat16)
    packed = jnp.concatenate([hidden_in, mix_high[None], mix_low[None], pad_rows], axis=0)
    full_rows = lax.all_gather(packed, "tp", axis=0)
    mix_pair = full_rows[:, seq_dev : seq_dev + 2].astype(jnp.float32)
    mix_full = jax.nn.sigmoid(mix_pair[:, 0] + mix_pair[:, 1]).reshape(1, -1)
    vmem = pl.BlockSpec(memory_space=pltpu.VMEM)
    anywhere = pl.BlockSpec(memory_space=pltpu.HBM)
    smem = pl.BlockSpec(memory_space=pltpu.SMEM)
    heads_out, new_state = pl.pallas_call(
        attend,
        out_shape=(
            whole((seq_dev, local_heads * value_dim), jnp.bfloat16),
            whole(state_in.shape, jnp.float32),
        ),
        in_specs=[smem] + [vmem] * 6 + [anywhere] * 5,
        out_specs=(vmem, anywhere),
        scratch_shapes=[pltpu.VMEM(w_query.shape, jnp.bfloat16)] * 2
        + [pltpu.VMEM(w_value.shape, jnp.bfloat16)] * 2
        + [pltpu.VMEM(state_in.shape, jnp.float32)] * 2
        + [
            pltpu.SemaphoreType.DMA((4,)),
            pltpu.SemaphoreType.DMA((local_heads,)),
            pltpu.SemaphoreType.DMA((local_heads,)),
        ],
        name="attend",
    )(
        tp_index.reshape(1),
        full_rows,
        attn_gain[None],
        w_beta.T,
        w_decay.T,
        decay_scale[None],
        head_gain[None],
        w_query,
        w_key,
        w_value,
        w_gate,
        state_in,
    )
    all_heads = lax.all_gather(heads_out, "tp", axis=1, tiled=True)
    mixed = (
        hidden_in.astype(jnp.float32)
        + jnp.dot(all_heads, w_output, preferred_element_type=jnp.float32)
    ).astype(jnp.bfloat16)
    ep_index = lax.axis_index("ep")
    cores = 2
    ny = tp_size // cores
    nx = ny if ep_size % ny == 0 else 1
    nz = ep_size // nx
    core_index = tp_index % cores
    y_index = tp_index // cores
    weight_high, weight_low = split_two(route_weight)
    top_count = expert_ids.shape[1]
    side = jnp.concatenate(
        [
            expert_ids.astype(jnp.bfloat16),
            weight_high,
            weight_low,
            jnp.zeros((seq_dev, 128 - 3 * top_count), jnp.bfloat16),
        ],
        axis=1,
    )
    loaded = jnp.concatenate([mixed, side], axis=1)
    column = jnp.concatenate(
        [loaded] + [flip(loaded, dz * nx, 0) for dz in range(1, nz)], axis=0
    )
    sides = [column[:, local_width:]]
    bare = column[:, :local_width]
    blocks = []
    for dx in range(nx):
        line = []
        for dy in range(ny):
            near = bare if dx + dy == 0 else flip(column if dy == 0 else bare, dx, dy * cores)
            if dx > 0 and dy == 0:
                sides.append(near[:, local_width:])
                near = near[:, :local_width]
            line.append(rejoin([near, flip(near, 0, 1)], core_index))
        line = [[line[dy][c] for dy in range(ny)] for c in range(cores)]
        line = [rejoin(part, y_index) for part in line]
        blocks.append(
            jnp.concatenate([line[c][y] for y in range(ny) for c in range(cores)], axis=1)
        )
    mixed_full = jnp.concatenate(blocks, axis=0)
    side_rows = jnp.concatenate(sides, axis=0).astype(jnp.float32)
    share_rows = 0.0
    for k in range(top_count):
        weight = (
            side_rows[:, top_count + k : top_count + k + 1]
            + side_rows[:, 2 * top_count + k : 2 * top_count + k + 1]
        )
        named = side_rows[:, k : k + 1] == ep_index.astype(jnp.float32)
        share_rows = share_rows + jnp.where(named, weight, 0.0)
    normed2 = root_norm(mixed_full, ffn_gain).astype(jnp.bfloat16)

    part = dense_gate.shape[1] // tp_size
    my_gate = lax.dynamic_slice_in_dim(dense_gate, tp_index * part, part, 1)
    my_up = lax.dynamic_slice_in_dim(dense_up, tp_index * part, part, 1)
    my_down = lax.dynamic_slice_in_dim(dense_down, tp_index * part, part, 0)

    def hidden(gate_weight, up_weight):
        gate_val = jnp.dot(normed2, gate_weight, preferred_element_type=jnp.float32)
        up_val = jnp.dot(normed2, up_weight, preferred_element_type=jnp.float32)
        return jax.nn.silu(gate_val) * up_val

    inner = hidden(expert_gate[0], expert_up[0]).astype(jnp.bfloat16)
    dense_hidden = hidden(my_gate, my_up).astype(jnp.bfloat16)
    total = (
        share_rows * jnp.dot(inner, expert_down[0], preferred_element_type=jnp.float32)
        + mix_full * jnp.dot(dense_hidden, my_down, preferred_element_type=jnp.float32)
    ).astype(jnp.bfloat16)

    lots = [
        [
            total[:, (y * cores + c) * local_width : (y * cores + c + 1) * local_width]
            for c in range(cores)
        ]
        for y in range(ny)
    ]
    near = []
    for pair in rejoin_all(lots, y_index):
        pair = rejoin(pair, core_index)
        over = flip(pair[1], 0, 1)
        near.append((pair[0].astype(jnp.float32) + over.astype(jnp.float32)).astype(jnp.bfloat16))
    span = nz * seq_dev
    summed = 0.0
    for dx in range(nx):
        for dy in range(ny):
            piece = near[dy][dx * span : (dx + 1) * span]
            piece = piece if dx + dy == 0 else flip(piece, dx, dy * cores)
            summed = summed + piece.astype(jnp.float32)
    summed = summed.astype(jnp.bfloat16)
    result = mixed.astype(jnp.float32)
    for dz in range(nz):
        piece = summed[dz * seq_dev : (dz + 1) * seq_dev]
        piece = piece if dz == 0 else flip(piece, dz * nx, 0)
        result = result + piece.astype(jnp.float32)
    return (result.astype(jnp.bfloat16), new_state)


def solution(mesh):
    placed = (
        P("ep", "tp"),
        P("ep", "tp", None, None),
        P(),
        P(None, "tp"),
        P(None, "tp"),
        P(None, "tp"),
        P(None, "tp"),
        P(),
        P(),
        P(),
        P(),
        P(None, "tp"),
        P(),
        P("ep", None),
        P("ep", None),
        P("ep", None, "tp"),
        P("ep", None, "tp"),
        P("ep", "tp", None),
        P(None, "ep"),
        P(None, "ep"),
        P("ep", None),
        P("tp"),
    )
    return jax.shard_map(
        per_device,
        mesh=mesh,
        in_specs=placed,
        out_specs=(P("ep", "tp"), P("ep", "tp", None, None)),
        check_vma=False,
    )
```
